32 devices in a mesh: sp: 16 (over z, y, x), tp: 2 (over core).
Axes of the slice: x: 2, y: 2, z: 4, core: 2. Of those that a mesh axis runs over, the one named last changes fastest.
Arguments:
- tokens: bfloat16 [4096, 4096], P('sp', 'tp'), may hold values from -480 to 480
- gain: float32 [4096], P('tp'), may hold values from 0.1 to 1.9
- q_att: bfloat16 [4096, 2048], P('sp', 'tp'), may hold values from -2.90625 to 2.90625
- k_att: bfloat16 [4096, 1024], P('sp', 'tp'), may hold values from -0.09375 to 0.09375
- v_att: bfloat16 [4096, 1024], P('sp', 'tp'), may hold values from -0.75 to 0.75
- q_ret: bfloat16 [4096, 1024], P('sp', 'tp'), may hold values from -0.09375 to 0.09375
- k_ret: bfloat16 [4096, 1024], P('sp', 'tp'), may hold values from -0.09375 to 0.09375
- v_ret: bfloat16 [4096, 1024], P('sp', 'tp'), may hold values from -0.09375 to 0.09375
- out_att: bfloat16 [2048, 4096], P('tp', 'sp'), may hold values from -0.109375 to 0.109375
- out_ret: bfloat16 [1024, 4096], P('tp', 'sp'), may hold values from -0.109375 to 0.109375
- sink: float32 [16], P('tp'), may hold values from 3 to 7
- decay_log: float32 [8, 4096], P('tp', 'sp'), may hold values from -2.125 to 0
Outputs:
- mixed: bfloat16 [4096, 4096], P(('sp', 'tp'))
- log_weight: float32 [16, 4096], P('tp', 'sp')
The draws below stay inside these ranges and needn't reach their ends.
All inputs are finite; a program needn't handle non-finite values.
Results may differ from the reference program's by a relative error of at most 0.017.
Values may be sent and summed in bfloat16 or wider, within the bound.
A program may use at most 128 MiB of HBM per device.

```python
import jax
import jax.numpy as jnp
from jax import lax

D = 4096
ATT_HEADS = 16
KV_HEADS = 8
RET_HEADS = 8
HEAD_DIM = 128
SPAN_RADIUS = 128
TOK_DEV = 256
TOKENS = 4096
N_TP = 2


def drawn_pair(key):
    base = jax.random.fold_in(key, 31)
    lookup_fraction = jnp.clip(jax.random.normal(jax.random.fold_in(base, 1), (D, KV_HEADS * HEAD_DIM), jnp.float32), -6.0, 6.0) * D ** (-0.5)
    query_part = jnp.clip(jax.random.normal(jax.random.fold_in(base, 2), (D, ATT_HEADS * HEAD_DIM), jnp.float32), -6.0, 6.0) * D ** (-0.5)
    return (query_part, lookup_fraction)


def draw_q_att(key, part):
    return drawn_pair(key)[0].astype(jnp.bfloat16)


def draw_k_att(key, part):
    return drawn_pair(key)[1].astype(jnp.bfloat16)


def draw_tokens(key, part):
    normal_part = jnp.clip(jax.random.normal(jax.random.fold_in(key, 41), (TOKENS, D), jnp.float32), -6.0, 6.0)
    column = jnp.arange(D).astype(jnp.float32) / D
    course = 2.0 * (jnp.arange(TOKENS).astype(jnp.float32) + 0.5) / TOKENS - 1.0
    direction = jax.random.uniform(jax.random.fold_in(key, 43), (1, D), jnp.float32, -1.0, 1.0)
    drift = jnp.exp(1.2 * direction * course[:, None])
    scale = drift * (4.0 ** column)[None, :]
    return (normal_part * scale).astype(jnp.bfloat16)


def draw_decay_log(key, part):
    blocks = TOKENS // TOK_DEV
    share = 0.5
    fast = jax.random.uniform(jax.random.fold_in(key, 51), (RET_HEADS, 1), jnp.float32) < share
    fast_rate = jax.random.uniform(jax.random.fold_in(key, 52), (RET_HEADS, 1), jnp.float32, 10.0, 16.0) / TOK_DEV
    slow_rate = jax.random.uniform(jax.random.fold_in(key, 53), (RET_HEADS, 1), jnp.float32, 0.1, 0.3) / TOKENS
    fading_pace = jnp.where(fast, fast_rate, slow_rate)
    scaling_factor = jnp.exp(jax.random.uniform(jax.random.fold_in(key, 54), (RET_HEADS, blocks), jnp.float32, jnp.log(0.5), jnp.log(2.0)))
    scaling_factor = jnp.repeat(scaling_factor, TOK_DEV, axis=1)
    spots = jax.random.randint(jax.random.fold_in(key, 55), (2,), 0, TOKENS)
    agreement_tally = (jnp.arange(TOKENS)[None, :] == spots[:, None]).astype(jnp.float32)
    discarded_entries = jnp.log(jax.random.uniform(jax.random.fold_in(key, 56), (2, RET_HEADS), jnp.float32, 0.5, 0.8))
    clustered_lists = jnp.dot(discarded_entries.T, agreement_tally)
    return -fading_pace * scaling_factor + clustered_lists


def steps_of(key, dims, cuts, least, largest):
    loudness, own = 1.0, jax.random.fold_in(key, 6)
    for axis_at, shards_of in cuts:
        heights = jnp.exp(jax.random.uniform(jax.random.fold_in(own, axis_at), (shards_of,), jnp.float32, least / len(cuts), largest / len(cuts)))
        loudness = loudness * jnp.repeat(heights, dims[axis_at] // shards_of).reshape([-1 if axis == axis_at else 1 for axis in range(len(dims))])
    return loudness


def scatter_about(key, extent, spread, reach, split=(), kind=jnp.bfloat16):
    values = jax.random.normal(key, extent, jnp.float32) * spread
    if len(split) > 0:
        values = steps_of(key, extent, split, -0.22, 0.18) * values
    return jnp.clip(values, min=-reach, max=reach).astype(kind)


def setup_inputs(seed: int = 0) -> dict:
    streams_of = jax.random.split(jax.random.key(seed), 13)
    return {
        "tokens": draw_tokens(jax.random.fold_in(streams_of[12], 71), 0),
        "gain": jnp.clip(1.0 + 0.18 * jax.random.normal(streams_of[1], (D,), jnp.float32), 0.1, 1.9),
        "q_att": draw_q_att(jax.random.fold_in(streams_of[12], 71), 0),
        "k_att": draw_k_att(jax.random.fold_in(streams_of[12], 71), 0),
        "v_att": scatter_about(streams_of[4], (D, KV_HEADS * HEAD_DIM), (max(D // 64, 1)) ** -0.5, 0.75, ((0, 16), (1, 2))),
        "q_ret": scatter_about(streams_of[5], (D, RET_HEADS * HEAD_DIM), D ** -0.5, 0.09375, ((0, 16), (1, 2))),
        "k_ret": scatter_about(streams_of[6], (D, RET_HEADS * HEAD_DIM), D ** -0.5, 0.09375, ((0, 16), (1, 2))),
        "v_ret": scatter_about(streams_of[7], (D, RET_HEADS * HEAD_DIM), D ** -0.5, 0.09375, ((0, 16), (1, 2))),
        "out_att": scatter_about(streams_of[8], (ATT_HEADS * HEAD_DIM, D), ((ATT_HEADS + RET_HEADS) * HEAD_DIM) ** -0.5, 0.109375, ((0, 2), (1, 16))),
        "out_ret": scatter_about(streams_of[9], (RET_HEADS * HEAD_DIM, D), ((ATT_HEADS + RET_HEADS) * HEAD_DIM) ** -0.5, 0.109375, ((0, 2), (1, 16))),
        "sink": jnp.clip(3.0 + 4.0 * jax.random.uniform(streams_of[10], (ATT_HEADS,), jnp.float32) ** steps_of(streams_of[10], (ATT_HEADS,), ((0, 2),), -0.2, 0.2), 3.0, 7.0),
        "decay_log": draw_decay_log(jax.random.fold_in(streams_of[12], 71), 0),
    }


def rotate(values, angles):
    half = values.shape[-1] // 2
    first = values[..., :half]
    second = values[..., half:]
    cosine = jnp.cos(angles)[:, None, :]
    sine = jnp.sin(angles)[:, None, :]
    return jnp.concatenate([first * cosine - second * sine, second * cosine + first * sine], axis=-1)

def angle_table(positions):
    freqs = 10000.0 ** (-jnp.arange(0, HEAD_DIM, 2).astype(jnp.float32) / HEAD_DIM)
    return positions[:, None] * freqs[None, :]

def window_attention(queries, padded_keys, padded_values, sink_logit, offset, total_rows, block_rows):
    count = queries.shape[0] // block_rows
    nearby_memory = queries.shape[1]
    group = queries.shape[2]

    def single_block(index):
        begin = index * block_rows
        block_query = lax.dynamic_slice_in_dim(queries, begin, block_rows, 0).astype(jnp.float32)
        block_keys = lax.dynamic_slice_in_dim(padded_keys, begin, block_rows + 2 * SPAN_RADIUS, 0).astype(jnp.float32)
        block_values = lax.dynamic_slice_in_dim(padded_values, begin, block_rows + 2 * SPAN_RADIUS, 0).astype(jnp.float32)
        scores = jnp.einsum('qhgd,khd->hgqk', block_query, block_keys) * HEAD_DIM ** (-0.5)
        query_pos = offset + begin + jnp.arange(block_rows, dtype=jnp.int32)
        key_pos = offset + begin - SPAN_RADIUS + jnp.arange(block_rows + 2 * SPAN_RADIUS, dtype=jnp.int32)
        spacing = key_pos[None, :] - query_pos[:, None]
        valid = (jnp.abs(spacing) <= SPAN_RADIUS) & (key_pos >= 0)[None, :] & (key_pos < total_rows)[None, :]
        masked = jnp.where(valid, scores, -jnp.inf)
        top = jnp.maximum(lax.optimization_barrier(jnp.max(masked, axis=-1)), sink_logit[:, :, None])
        expo = jnp.exp(masked - top[..., None])
        total = lax.optimization_barrier(jnp.sum(expo, axis=-1)) + jnp.exp(sink_logit[:, :, None] - top)
        logs = top + jnp.log(total)
        probs = (expo / total[..., None]).astype(jnp.bfloat16)
        result = jnp.einsum('hgqk,khd->qhgd', probs.astype(jnp.float32), block_values).astype(jnp.bfloat16)
        return (result.reshape(block_rows, nearby_memory * group * HEAD_DIM), logs.reshape(nearby_memory * group, block_rows))
    outs, logs = lax.map(single_block, jnp.arange(count, dtype=jnp.int32))
    return (outs.reshape(queries.shape[0], -1), jnp.moveaxis(logs, 0, 1).reshape(logs.shape[1], -1))

def retention(queries, keys, values, decay):
    blocks = queries.shape[0] // TOK_DEV
    heads = queries.shape[1]
    highest = lax.Precision.HIGHEST
    query_b = queries.reshape(blocks, TOK_DEV, heads, HEAD_DIM)
    key_b = keys.reshape(blocks, TOK_DEV, heads, HEAD_DIM)
    value_b = values.reshape(blocks, TOK_DEV, heads, HEAD_DIM)
    decay_b = jnp.moveaxis(decay.reshape(heads, blocks, TOK_DEV), 1, 0)

    def local(items):
        query_f = items[0].astype(jnp.float32)
        key_f = items[1].astype(jnp.float32)
        value_f = items[2].astype(jnp.float32)
        cumul = jnp.cumsum(items[3], axis=1)
        last = cumul[:, -1]
        scores = jnp.einsum('qhd,khd->hqk', query_f, key_f)
        weights = jnp.exp(-jnp.abs(cumul[:, :, None] - cumul[:, None, :]))
        inner = jnp.einsum('hqk,khd->qhd', scores * weights, value_f, precision=highest)
        forward = jnp.einsum('hk,khd,khe->hde', jnp.exp(last[:, None] - cumul), key_f, value_f, precision=highest)
        backward = jnp.einsum('hk,khd,khe->hde', jnp.exp(cumul), key_f, value_f, precision=highest)
        return (inner, forward, backward, jnp.exp(last), cumul)
    inner, forward, backward, totals, cumuls = lax.map(local, (query_b, key_b, value_b, decay_b))

    def step(carry, item):
        return (item[0][:, None, None] * carry + item[1], carry)
    zero = jnp.zeros(forward.shape[1:], jnp.float32)
    _, before = lax.scan(step, zero, (totals, forward))
    _, after = lax.scan(step, zero, (totals, backward), reverse=True)
    query_f = query_b.astype(jnp.float32)
    lead = jnp.moveaxis(jnp.exp(cumuls), 1, 2)[..., None]
    trail = jnp.moveaxis(jnp.exp(cumuls[:, :, -1:] - cumuls), 1, 2)[..., None]
    carried = lead * jnp.einsum('bqhd,bhde->bqhe', query_f, before, precision=highest)
    carried = carried + trail * jnp.einsum('bqhd,bhde->bqhe', query_f, after, precision=highest)
    blended_output = inner + carried
    middle_point = blended_output - lax.optimization_barrier(jnp.mean(blended_output, axis=-1, keepdims=True))
    normed = middle_point * lax.rsqrt(lax.optimization_barrier(jnp.mean(middle_point * middle_point, axis=-1, keepdims=True)) + 1e-06)
    return normed.astype(jnp.bfloat16).reshape(queries.shape[0], heads * HEAD_DIM)

def reference(tokens, gain, q_att, k_att, v_att, q_ret, k_ret, v_ret, out_att, out_ret, sink, decay_log):
    widened = tokens.astype(jnp.float32)
    inverse = lax.rsqrt(lax.optimization_barrier(jnp.sum(widened * widened, axis=1)) / D + 1e-06)[:, None]
    scaled = (widened * gain).astype(jnp.bfloat16)

    def project(weight):
        return jnp.dot(scaled, weight, preferred_element_type=jnp.float32) * inverse
    angles = angle_table(jnp.arange(TOKENS).astype(jnp.float32))
    group = ATT_HEADS // KV_HEADS
    att_query = rotate(project(q_att).reshape(TOKENS, ATT_HEADS, HEAD_DIM), angles).astype(jnp.bfloat16)
    att_key = rotate(project(k_att).reshape(TOKENS, KV_HEADS, HEAD_DIM), angles).astype(jnp.bfloat16)
    att_value = project(v_att).astype(jnp.bfloat16).reshape(TOKENS, KV_HEADS, HEAD_DIM)
    padding = ((SPAN_RADIUS, SPAN_RADIUS), (0, 0), (0, 0))
    att_out, log_weight = window_attention(att_query.reshape(TOKENS, KV_HEADS, group, HEAD_DIM), jnp.pad(att_key, padding), jnp.pad(att_value, padding), sink.reshape(KV_HEADS, group), 0, TOKENS, min(TOK_DEV, 512))
    ret_query = project(q_ret).astype(jnp.bfloat16).reshape(TOKENS, RET_HEADS, HEAD_DIM)
    ret_key = (jnp.dot(scaled, k_ret, preferred_element_type=jnp.float32) * (inverse * HEAD_DIM ** (-0.5))).astype(jnp.bfloat16).reshape(TOKENS, RET_HEADS, HEAD_DIM)
    ret_value = project(v_ret).astype(jnp.bfloat16).reshape(TOKENS, RET_HEADS, HEAD_DIM)
    ret_out = retention(ret_query, ret_key, ret_value, decay_log)
    att_width = ATT_HEADS * HEAD_DIM // N_TP
    ret_width = RET_HEADS * HEAD_DIM // N_TP
    summed = jnp.zeros((TOKENS, D), jnp.float32)
    for member in range(N_TP):
        term = jnp.dot(att_out[:, member * att_width:(member + 1) * att_width], out_att[member * att_width:(member + 1) * att_width], preferred_element_type=jnp.float32)
        term = term + jnp.dot(ret_out[:, member * ret_width:(member + 1) * ret_width], out_ret[member * ret_width:(member + 1) * ret_width], preferred_element_type=jnp.float32)
        summed = summed + lax.optimization_barrier(term.astype(jnp.bfloat16)).astype(jnp.float32)
    return (summed.astype(jnp.bfloat16), log_weight)
```

```python
import math

import jax
import jax.numpy as jnp
from jax import lax
from jax.sharding import Mesh
from jax.sharding import PartitionSpec as P

HEAD_DIM = 128
SPAN_RADIUS = 128
BLOCK = 256
HIGHEST = lax.Precision.HIGHEST


def gather(x, axis, dim):
    if lax.axis_size(axis) == 1:
        return x
    return lax.all_gather(x, axis, axis=dim, tiled=True)


def exchange(x, axis, split, concat):
    if lax.axis_size(axis) == 1:
        return x
    return lax.all_to_all(x, axis, split, concat, tiled=True)


def halo(shard, axis, width):
    peers, length = lax.axis_size(axis), shard.shape[1]
    up = [(i, i + 1) for i in range(peers - 1)]
    down = [(j, i) for i, j in up]
    before = lax.ppermute(shard[:, length - width :], axis, up)
    after = lax.ppermute(shard[:, :width], axis, down)
    return jnp.concatenate([before, shard, after], axis=1)


def rotate(values, cosine, sine):
    half = values.shape[-1] // 2
    first, second = values[..., :half], values[..., half:]
    return jnp.concatenate(
        [first * cosine - second * sine, second * cosine + first * sine], axis=-1
    ).astype(jnp.bfloat16)


def attend(query, key, value, sink, offset, total_rows):
    rows, kv, group, _ = query.shape
    ext = halo(jnp.stack([key, value]), "t", SPAN_RADIUS)
    size = min(rows, BLOCK)
    count = rows // size
    span = size + 2 * SPAN_RADIUS
    pieces = jnp.stack([ext[:, b * size : b * size + span] for b in range(count)])
    blocks = query.reshape(count, size, kv, group, HEAD_DIM)
    scores = jnp.einsum(
        "bqhgd,bkhd->bhgqk", blocks, pieces[:, 0], preferred_element_type=jnp.float32
    ) * HEAD_DIM ** (-0.5)
    base = offset + jnp.arange(count, dtype=jnp.int32) * size
    query_pos = base[:, None] + jnp.arange(size, dtype=jnp.int32)
    key_pos = base[:, None] - SPAN_RADIUS + jnp.arange(span, dtype=jnp.int32)
    spacing = key_pos[:, None, :] - query_pos[:, :, None]
    inside = (key_pos >= 0) & (key_pos < total_rows)
    valid = (jnp.abs(spacing) <= SPAN_RADIUS) & inside[:, None, :]
    masked = jnp.where(valid[:, None, None], scores, -jnp.inf)
    limit = sink[None, :, :, None]
    top = jnp.maximum(jnp.max(masked, axis=-1), limit)
    expo = jnp.exp(masked - top[..., None])
    total = jnp.sum(expo, axis=-1) + jnp.exp(limit - top)
    logs = top + jnp.log(total)
    probs = (expo / total[..., None]).astype(jnp.bfloat16)
    result = jnp.einsum(
        "bhgqk,bkhd->bqhgd", probs, pieces[:, 1], preferred_element_type=jnp.float32
    ).astype(jnp.bfloat16)
    logs = jnp.transpose(logs, (1, 2, 0, 3)).reshape(kv * group, rows)
    return result.reshape(rows, kv * group * HEAD_DIM), logs


def retain(query, key, value, decay):
    rows, heads, _ = query.shape
    peers, index = lax.axis_size("t"), lax.axis_index("t")
    cumul = jnp.cumsum(decay, axis=1)
    last = cumul[:, -1]
    query_f, key_f, value_f = (v.astype(jnp.float32) for v in (query, key, value))
    trailing = jnp.exp(last[:, None] - cumul)
    leading = jnp.exp(cumul)
    forward = jnp.einsum("hk,khd,khe->hde", trailing, key_f, value_f, precision=HIGHEST)
    backward = jnp.einsum("hk,khd,khe->hde", leading, key_f, value_f, precision=HIGHEST)
    tail = jnp.broadcast_to(last[:, None, None], (heads, 8, HEAD_DIM))
    sent = jnp.concatenate([forward, backward, tail], axis=1)
    seen = lax.all_gather(sent, "t", axis=0)
    lasts = seen[:, :, 2 * HEAD_DIM, 0]
    at = jnp.arange(peers)
    low = jnp.minimum(at, index)[:, None]
    high = jnp.maximum(at, index)[:, None]
    between = (at[None, :] > low) & (at[None, :] < high)
    spans = jnp.exp(jnp.sum(jnp.where(between[:, :, None], lasts[None], 0.0), axis=1))
    before = jnp.sum(
        jnp.where(at < index, 1.0, 0.0)[:, None, None, None]
        * spans[:, :, None, None]
        * seen[:, :, :HEAD_DIM],
        axis=0,
    )
    after = jnp.sum(
        jnp.where(at > index, 1.0, 0.0)[:, None, None, None]
        * spans[:, :, None, None]
        * seen[:, :, HEAD_DIM : 2 * HEAD_DIM],
        axis=0,
    )
    scores = jnp.einsum("qhd,khd->hqk", query, key, preferred_element_type=jnp.float32)
    weights = jnp.exp(-jnp.abs(cumul[:, :, None] - cumul[:, None, :]))
    mix = jnp.einsum("hqk,khd->qhd", scores * weights, value_f, precision=HIGHEST)
    mix = mix + leading.T[:, :, None] * jnp.einsum(
        "qhd,hde->qhe", query_f, before, precision=HIGHEST
    )
    mix = mix + trailing.T[:, :, None] * jnp.einsum(
        "qhd,hde->qhe", query_f, after, precision=HIGHEST
    )
    middle = mix - jnp.mean(mix, axis=-1, keepdims=True)
    normed = middle * lax.rsqrt(jnp.mean(middle * middle, axis=-1, keepdims=True) + 1e-06)
    return normed.astype(jnp.bfloat16).reshape(rows, heads * HEAD_DIM)


def shards(
    tokens, gain, q_att, k_att, v_att, q_ret, k_ret, v_ret, out_att, out_ret, sink, decay_log
):
    parts = lax.axis_size("h")
    own = tokens.shape[0]
    rows = own * parts
    width = tokens.shape[1] * lax.axis_size("tp")
    kv = k_att.shape[1] // HEAD_DIM // parts
    group = q_att.shape[1] // k_att.shape[1]
    att = kv * group
    ret = q_ret.shape[1] // HEAD_DIM // parts
    offset = lax.axis_index("t") * rows
    total_rows = rows * lax.axis_size("t")

    packed = jnp.concatenate(
        [
            w.reshape(w.shape[0], parts, w.shape[1] // parts)
            for w in (q_att, k_att, v_att, q_ret, k_ret, v_ret)
        ],
        axis=2,
    )
    packed = jnp.moveaxis(packed, 1, 0).reshape(parts * packed.shape[0], packed.shape[2])
    weight = gather(exchange(packed, "h", 0, 0), "t", 0)

    widened = tokens.astype(jnp.float32)
    sums = lax.all_gather(jnp.sum(widened * widened, axis=1), ("h", "tp"))
    squares = jnp.sum(sums.reshape(parts, lax.axis_size("tp"), own), axis=1).reshape(rows)
    inverse = lax.rsqrt(squares / width + 1e-06)[:, None]
    scaled = (widened * gain).astype(jnp.bfloat16)
    whole = gather(gather(scaled, "h", 0), "tp", 1)
    proj = jnp.dot(whole, weight, preferred_element_type=jnp.float32)

    edges = [att, kv, kv, ret, ret, ret]
    starts = [sum(edges[:i]) * HEAD_DIM for i in range(6)]
    qa, ka, va, qr, kr, vr = (
        proj[:, s : s + n * HEAD_DIM].reshape(rows, n, HEAD_DIM) for s, n in zip(starts, edges)
    )
    scale = inverse[:, :, None]
    positions = (offset + jnp.arange(rows, dtype=jnp.int32)).astype(jnp.float32)
    freqs = 10000.0 ** (-jnp.arange(0, HEAD_DIM, 2).astype(jnp.float32) / HEAD_DIM)
    angles = positions[:, None] * freqs[None, :]
    cosine, sine = jnp.cos(angles)[:, None, :], jnp.sin(angles)[:, None, :]
    att_query = rotate(qa * scale, cosine, sine)
    att_key = rotate(ka * scale, cosine, sine)
    att_value = (va * scale).astype(jnp.bfloat16)
    ret_query = (qr * scale).astype(jnp.bfloat16)
    ret_key = (kr * (scale * HEAD_DIM ** (-0.5))).astype(jnp.bfloat16)
    ret_value = (vr * scale).astype(jnp.bfloat16)

    logits = lax.dynamic_slice_in_dim(sink, lax.axis_index("h") * att, att).reshape(kv, group)
    att_out, logs = attend(
        att_query.reshape(rows, kv, group, HEAD_DIM), att_key, att_value, logits, offset, total_rows
    )
    ret_out = retain(ret_query, ret_key, ret_value, exchange(decay_log, "h", 0, 1))

    out_pack = jnp.concatenate(
        [w.reshape(parts, w.shape[0] // parts, w.shape[1]) for w in (out_att, out_ret)], axis=1
    )
    out_wide = gather(exchange(out_pack, "h", 0, 0), "t", 0)
    depth = out_wide.shape[1]
    out_wide = jnp.moveaxis(out_wide, 0, 1).reshape(depth, -1)
    mixed = jnp.dot(
        jnp.concatenate([att_out, ret_out], axis=1), out_wide, preferred_element_type=jnp.float32
    ).astype(jnp.bfloat16)
    mixed = lax.psum_scatter(mixed, ("h", "tp"), scatter_dimension=0, tiled=True)
    return mixed, exchange(logs, "h", 1, 0)


def solution(mesh):
    sp, tp = mesh.shape["sp"], mesh.shape["tp"]

    def run(*args):
        heads = math.gcd(args[3].shape[1], args[5].shape[1]) // HEAD_DIM
        parts = math.gcd(heads // math.gcd(heads, tp), sp)
        fine = Mesh(mesh.devices.reshape(sp // parts, parts, tp), ("t", "h", "tp"))
        seq = ("t", "h")
        body = jax.shard_map(
            shards,
            mesh=fine,
            in_specs=(P(seq, "tp"), P("tp"))
            + (P(seq, "tp"),) * 6
            + (P("tp", seq), P("tp", seq), P("tp"), P("tp", seq)),
            out_specs=(P(("t", "h", "tp"), None), P("tp", seq)),
            check_vma=False,
        )
        return body(*args)

    return run
```

```python
import functools
import math

import jax
import jax.numpy as jnp
from jax import lax
from jax.experimental import pallas as pl
from jax.experimental.pallas import tpu as pltpu
from jax.sharding import Mesh
from jax.sharding import PartitionSpec as P

HEAD_DIM = 128
SPAN_RADIUS = 128
BLOCK = 256
HIGHEST = lax.Precision.HIGHEST
MESH = pl.DeviceIdType.MESH


def gather(x, axis, dim):
    if lax.axis_size(axis) == 1:
        return x
    return lax.all_gather(x, axis, axis=dim, tiled=True)


def exchange(x, axis, split, concat):
    if lax.axis_size(axis) == 1:
        return x
    return lax.all_to_all(x, axis, split, concat, tiled=True)


def halo(shard, axis, width):
    peers, length = lax.axis_size(axis), shard.shape[1]
    up = [(i, i + 1) for i in range(peers - 1)]
    down = [(j, i) for i, j in up]
    before = lax.ppermute(shard[:, length - width :], axis, up)
    after = lax.ppermute(shard[:, :width], axis, down)
    return jnp.concatenate([before, shard, after], axis=1)


def rotate(values, cosine, sine):
    half = values.shape[-1] // 2
    first, second = values[..., :half], values[..., half:]
    return jnp.concatenate(
        [first * cosine - second * sine, second * cosine + first * sine], axis=-1
    ).astype(jnp.bfloat16)


def front_kernel(
    peers, parts, cores,
    packed, scaled, sums, outp, decay,
    proj, out_all, sums_all, decay_all,
    wide, seen,
    w_recv, up_send, down_send, w_send,
    x_recv, x_send, swap_send,
    s_recv, s_send, o_recv, o_send, d_recv, d_send, local,
):
    t, h, c = lax.axis_index("t"), lax.axis_index("h"), lax.axis_index("tp")
    blocks, own, _ = scaled.shape

    def other(d):
        return lax.rem(h + d, parts)

    def source(d):
        return lax.rem(h - d + parts, parts)

    barrier = pltpu.get_barrier_semaphore()
    for d in range(parts):
        for e in range(cores):
            if d or e:
                pl.semaphore_signal(
                    barrier,
                    inc=1,
                    device_id={"h": other(d), "tp": lax.rem(c + e, cores)},
                    device_id_type=MESH,
                )

    for d in range(1, peers):
        pl.semaphore_signal(
            barrier, inc=1, device_id={"t": lax.rem(t + d, peers)}, device_id_type=MESH
        )
    pl.semaphore_wait(barrier, parts * cores + peers - 2)

    def remote(src, dst, send, recv, where):
        return pltpu.make_async_remote_copy(
            src_ref=src, dst_ref=dst, send_sem=send, recv_sem=recv,
            device_id=where, device_id_type=MESH,
        )

    def upward(b, p, src=None):
        return remote(
            wide.at[b, p] if src is None else src,
            wide.at[b, p], up_send.at[b, p], w_recv.at[b, p], {"t": t + 1},
        )

    def downward(b, p, src=None):
        return remote(
            wide.at[b, p] if src is None else src,
            wide.at[b, p], down_send.at[b, p], w_recv.at[b, p], {"t": t - 1},
        )

    def weight_to(d):
        return remote(
            packed.at[other(d)], wide.at[t, h], w_send.at[d], w_recv.at[t, h], {"h": other(d)}
        )

    def place(p, e):
        return seen.at[pl.ds(e * blocks, blocks), pl.ds(p * own, own)]

    def token_to(d):
        return remote(scaled, place(h, c), x_send.at[d], x_recv.at[h, c], {"h": other(d)})

    def swap(p, src):
        return remote(
            src, place(p, c), swap_send.at[p], x_recv.at[p, c], {"tp": lax.rem(c + 1, cores)}
        )

    def sum_to(d, e):
        return remote(
            sums, sums_all.at[h, c], s_send.at[d, e], s_recv.at[h, c],
            {"h": other(d), "tp": lax.rem(c + e, cores)},
        )

    def out_to(d):
        return remote(
            outp.at[other(d)], out_all.at[h], o_send.at[d], o_recv.at[h], {"h": other(d)}
        )

    def decay_to(d):
        return remote(
            decay.at[other(d)], decay_all.at[h], d_send.at[d], d_recv.at[h], {"h": other(d)}
        )

    for d in range(1, parts):
        weight_to(d).start()

    @pl.when(t < peers - 1)
    def _():
        upward(t, h, packed.at[h]).start()

    @pl.when(t > 0)
    def _():
        downward(t, h, packed.at[h]).start()

    for d in range(1, parts):
        token_to(d).start()
    swap(h, scaled).start()
    for d in range(1, parts):
        decay_to(d).start()
        out_to(d).start()
    for d in range(parts):
        for e in range(cores):
            if d or e:
                sum_to(d, e).start()
    mine = (
        pltpu.make_async_copy(packed.at[h], wide.at[t, h], local.at[0]),
        pltpu.make_async_copy(scaled, place(h, c), local.at[1]),
        pltpu.make_async_copy(sums, sums_all.at[h, c], local.at[2]),
        pltpu.make_async_copy(outp.at[h], out_all.at[h], local.at[3]),
        pltpu.make_async_copy(decay.at[h], decay_all.at[h], local.at[4]),
    )
    for copy in mine:
        copy.start()
    proj[...] = jnp.zeros_like(proj)

    @pl.loop(1, parts)
    def _(d):
        p = source(d)
        upward(t, p).wait_recv()

        @pl.when(t < peers - 1)
        def _():
            upward(t, p).start()

        @pl.when(t > 0)
        def _():
            downward(t, p).start()

    def relay(s, d):
        p = source(d)

        @pl.when(t - s >= 0)
        def _():
            upward(t - s, p).wait_recv()

            @pl.when(t < peers - 1)
            def _():
                upward(t - s, p).start()

        @pl.when(t + s < peers)
        def _():
            downward(t + s, p).wait_recv()

            @pl.when(t > 0)
            def _():
                downward(t + s, p).start()

    @pl.loop(0, parts)
    def _(d):
        relay(1, d)

        @pl.when(d < parts - 1)
        def _():
            p = source(d + 1)
            swap(p, place(p, c)).wait_recv()
            swap(p, place(p, c)).start()

    for copy in mine:
        copy.wait()

    @pl.loop(0, parts)
    def _(p):
        e = lax.rem(c + 1, cores)
        pltpu.make_async_remote_copy(
            src_ref=place(p, e), dst_ref=place(p, e),
            send_sem=swap_send.at[p], recv_sem=x_recv.at[p, e],
            device_id={"tp": e}, device_id_type=MESH,
        ).wait_recv()

    def add(b, p):
        @pl.loop(0, parts)
        def _(r):
            at = pl.ds(pl.multiple_of(r * own, own), own)
            proj[at, :] += jnp.dot(
                seen[b * parts + p, at, :], wide[b, p], preferred_element_type=jnp.float32
            )

    @pl.loop(0, peers)
    def _(s):
        @pl.loop(0, parts)
        def _(d):
            p = source(d)

            @pl.when(s >= 2)
            def _():
                relay(s, d)

            @pl.when(t - s >= 0)
            def _():
                add(t - s, p)

            @pl.when((s > 0) & (t + s < peers))
            def _():
                add(t + s, p)

    @pl.loop(0, peers)
    def _(b):
        @pl.loop(0, parts)
        def _(p):
            @pl.when((b <= t) & (t < peers - 1))
            def _():
                upward(b, p).wait_send()

            @pl.when((b >= t) & (t > 0))
            def _():
                downward(b, p).wait_send()

    for p in range(parts):
        swap(p, place(p, c)).wait_send()
    for d in range(parts):
        if d:
            p = source(d)
            weight_to(d).wait_send()
            token_to(d).wait_send()
            out_to(d).wait_send()
            decay_to(d).wait_send()
            remote(
                outp.at[h], out_all.at[p], o_send.at[d], o_recv.at[p], {"h": p}
            ).wait_recv()
            remote(
                decay.at[h], decay_all.at[p], d_send.at[d], d_recv.at[p], {"h": p}
            ).wait_recv()
        for e in range(cores):
            if d or e:
                p, q = source(d), lax.rem(c + e, cores)
                sum_to(d, e).wait_send()
                remote(
                    sums, sums_all.at[p, q], s_send.at[d, e], s_recv.at[p, q],
                    {"h": p, "tp": q},
                ).wait_recv()


def front(packed, scaled, sums, outp, decay):
    peers, parts, cores = (lax.axis_size(a) for a in ("t", "h", "tp"))
    own, columns = packed.shape[1:]
    dma = pltpu.SemaphoreType.DMA
    vmem = pl.BlockSpec(memory_space=pltpu.VMEM)
    rows = parts * own
    return pl.pallas_call(
        functools.partial(front_kernel, peers, parts, cores),
        out_shape=(
            jax.ShapeDtypeStruct((rows, columns), jnp.float32),
            jax.ShapeDtypeStruct(outp.shape, outp.dtype),
            jax.ShapeDtypeStruct((parts, cores) + sums.shape, sums.dtype),
            jax.ShapeDtypeStruct(decay.shape, decay.dtype),
        ),
        in_specs=[vmem] * 5,
        out_specs=[vmem] * 4,
        scratch_shapes=[
            pltpu.VMEM((peers, parts, own, columns), jnp.bfloat16),
            pltpu.VMEM((cores * scaled.shape[0], rows, own), jnp.bfloat16),
            dma((peers, parts)), dma((peers, parts)), dma((peers, parts)), dma((parts,)),
            dma((parts, cores)), dma((parts,)), dma((parts,)),
            dma((parts, cores)), dma((parts, cores)),
            dma((parts,)), dma((parts,)), dma((parts,)), dma((parts,)), dma((5,)),
        ],
        compiler_params=pltpu.CompilerParams(
            collective_id=0, has_side_effects=True, vmem_limit_bytes=56 * 2**20
        ),
        cost_estimate=pl.CostEstimate(
            flops=10**11, bytes_accessed=2 * 10**7, transcendentals=0
        ),
    )(packed, scaled, sums, outp, decay)


def attend(query, key, value, sink, offset, total_rows):
    rows, kv, group, _ = query.shape
    ext = halo(jnp.stack([key, value]), "t", SPAN_RADIUS)
    size = min(rows, BLOCK)
    count = rows // size
    span = size + 2 * SPAN_RADIUS
    pieces = jnp.stack([ext[:, b * size : b * size + span] for b in range(count)])
    blocks = query.reshape(count, size, kv, group, HEAD_DIM)
    scores = jnp.einsum(
        "bqhgd,bkhd->bhgqk", blocks, pieces[:, 0], preferred_element_type=jnp.float32
    ) * HEAD_DIM ** (-0.5)
    base = offset + jnp.arange(count, dtype=jnp.int32) * size
    query_pos = base[:, None] + jnp.arange(size, dtype=jnp.int32)
    key_pos = base[:, None] - SPAN_RADIUS + jnp.arange(span, dtype=jnp.int32)
    spacing = key_pos[:, None, :] - query_pos[:, :, None]
    inside = (key_pos >= 0) & (key_pos < total_rows)
    valid = (jnp.abs(spacing) <= SPAN_RADIUS) & inside[:, None, :]
    masked = jnp.where(valid[:, None, None], scores, -jnp.inf)
    limit = sink[None, :, :, None]
    top = jnp.maximum(jnp.max(masked, axis=-1), limit)
    expo = jnp.exp(masked - top[..., None])
    total = jnp.sum(expo, axis=-1) + jnp.exp(limit - top)
    logs = top + jnp.log(total)
    probs = (expo / total[..., None]).astype(jnp.bfloat16)
    result = jnp.einsum(
        "bhgqk,bkhd->bqhgd", probs, pieces[:, 1], preferred_element_type=jnp.float32
    ).astype(jnp.bfloat16)
    logs = jnp.transpose(logs, (1, 2, 0, 3)).reshape(kv * group, rows)
    return result.reshape(rows, kv * group * HEAD_DIM), logs


def retain(query, key, value, decay):
    rows, heads, _ = query.shape
    peers, index = lax.axis_size("t"), lax.axis_index("t")
    cumul = jnp.cumsum(decay, axis=1)
    last = cumul[:, -1]
    query_f, key_f, value_f = (v.astype(jnp.float32) for v in (query, key, value))
    trailing = jnp.exp(last[:, None] - cumul)
    leading = jnp.exp(cumul)
    forward = jnp.einsum("hk,khd,khe->hde", trailing, key_f, value_f, precision=HIGHEST)
    backward = jnp.einsum("hk,khd,khe->hde", leading, key_f, value_f, precision=HIGHEST)
    tail = jnp.broadcast_to(last[:, None, None], (heads, 8, HEAD_DIM))
    sent = jnp.concatenate([forward, backward, tail], axis=1)
    seen = lax.all_gather(sent, "t", axis=0)
    lasts = seen[:, :, 2 * HEAD_DIM, 0]
    at = jnp.arange(peers)
    low = jnp.minimum(at, index)[:, None]
    high = jnp.maximum(at, index)[:, None]
    between = (at[None, :] > low) & (at[None, :] < high)
    spans = jnp.exp(jnp.sum(jnp.where(between[:, :, None], lasts[None], 0.0), axis=1))
    before = jnp.sum(
        jnp.where(at < index, 1.0, 0.0)[:, None, None, None]
        * spans[:, :, None, None]
        * seen[:, :, :HEAD_DIM],
        axis=0,
    )
    after = jnp.sum(
        jnp.where(at > index, 1.0, 0.0)[:, None, None, None]
        * spans[:, :, None, None]
        * seen[:, :, HEAD_DIM : 2 * HEAD_DIM],
        axis=0,
    )
    scores = jnp.einsum("qhd,khd->hqk", query, key, preferred_element_type=jnp.float32)
    weights = jnp.exp(-jnp.abs(cumul[:, :, None] - cumul[:, None, :]))
    mix = jnp.einsum("hqk,khd->qhd", scores * weights, value_f, precision=HIGHEST)
    mix = mix + leading.T[:, :, None] * jnp.einsum(
        "qhd,hde->qhe", query_f, before, precision=HIGHEST
    )
    mix = mix + trailing.T[:, :, None] * jnp.einsum(
        "qhd,hde->qhe", query_f, after, precision=HIGHEST
    )
    middle = mix - jnp.mean(mix, axis=-1, keepdims=True)
    normed = middle * lax.rsqrt(jnp.mean(middle * middle, axis=-1, keepdims=True) + 1e-06)
    return normed.astype(jnp.bfloat16).reshape(rows, heads * HEAD_DIM)


def shards(
    tokens, gain, q_att, k_att, v_att, q_ret, k_ret, v_ret, out_att, out_ret, sink, decay_log
):
    parts = lax.axis_size("h")
    own = tokens.shape[0]
    rows = own * parts
    width = tokens.shape[1] * lax.axis_size("tp")
    kv = k_att.shape[1] // HEAD_DIM // parts
    group = q_att.shape[1] // k_att.shape[1]
    att = kv * group
    ret = q_ret.shape[1] // HEAD_DIM // parts
    offset = lax.axis_index("t") * rows
    total_rows = rows * lax.axis_size("t")

    packed = jnp.concatenate(
        [
            w.reshape(w.shape[0], parts, w.shape[1] // parts)
            for w in (q_att, k_att, v_att, q_ret, k_ret, v_ret)
        ],
        axis=2,
    )
    packed = jnp.moveaxis(packed, 1, 0)
    out_pack = jnp.concatenate(
        [w.reshape(parts, w.shape[0] // parts, w.shape[1]) for w in (out_att, out_ret)], axis=1
    )
    widened = tokens.astype(jnp.float32)
    sums = jnp.sum(widened * widened, axis=1)
    scaled = (widened * gain).astype(jnp.bfloat16)
    cores = lax.axis_size("tp")
    if parts > 1 and cores == 2 and own % 128 == 0 and packed.shape[1] == own:
        tiles = jnp.moveaxis(scaled.reshape(own, -1, own), 1, 0)
        proj, out_own, sums, decay = front(
            packed, tiles, sums.reshape(-1, 128), out_pack, decay_log.reshape(parts, ret, own)
        )
        decay = jnp.moveaxis(decay, 0, 1).reshape(ret, rows)
    else:
        flat = packed.reshape(parts * packed.shape[1], packed.shape[2])
        weight = gather(exchange(flat, "h", 0, 0), "t", 0)
        whole = gather(gather(scaled, "h", 0), "tp", 1)
        proj = jnp.dot(whole, weight, preferred_element_type=jnp.float32)
        out_own = exchange(out_pack, "h", 0, 0)
        sums = lax.all_gather(sums, ("h", "tp"))
        decay = exchange(decay_log, "h", 0, 1)
    squares = jnp.sum(sums.reshape(parts, cores, own), axis=1).reshape(rows)
    inverse = lax.rsqrt(squares / width + 1e-06)[:, None]

    edges = [att, kv, kv, ret, ret, ret]
    starts = [sum(edges[:i]) * HEAD_DIM for i in range(6)]
    qa, ka, va, qr, kr, vr = (
        proj[:, s : s + n * HEAD_DIM].reshape(rows, n, HEAD_DIM) for s, n in zip(starts, edges)
    )
    scale = inverse[:, :, None]
    positions = (offset + jnp.arange(rows, dtype=jnp.int32)).astype(jnp.float32)
    freqs = 10000.0 ** (-jnp.arange(0, HEAD_DIM, 2).astype(jnp.float32) / HEAD_DIM)
    angles = positions[:, None] * freqs[None, :]
    cosine, sine = jnp.cos(angles)[:, None, :], jnp.sin(angles)[:, None, :]
    att_query = rotate(qa * scale, cosine, sine)
    att_key = rotate(ka * scale, cosine, sine)
    att_value = (va * scale).astype(jnp.bfloat16)
    ret_query = (qr * scale).astype(jnp.bfloat16)
    ret_key = (kr * (scale * HEAD_DIM ** (-0.5))).astype(jnp.bfloat16)
    ret_value = (vr * scale).astype(jnp.bfloat16)

    logits = lax.dynamic_slice_in_dim(sink, lax.axis_index("h") * att, att).reshape(kv, group)
    att_out, logs = attend(
        att_query.reshape(rows, kv, group, HEAD_DIM), att_key, att_value, logits, offset, total_rows
    )
    ret_out = retain(ret_query, ret_key, ret_value, decay)

    out_wide = gather(out_own, "t", 0)
    depth = out_wide.shape[1]
    out_wide = jnp.moveaxis(out_wide, 0, 1).reshape(depth, -1)
    mixed = jnp.dot(
        jnp.concatenate([att_out, ret_out], axis=1), out_wide, preferred_element_type=jnp.float32
    ).astype(jnp.bfloat16)
    mixed = lax.psum_scatter(mixed, ("h", "tp"), scatter_dimension=0, tiled=True)
    return mixed, exchange(logs, "h", 1, 0)


def solution(mesh):
    sp, tp = mesh.shape["sp"], mesh.shape["tp"]

    def run(*args):
        heads = math.gcd(args[3].shape[1], args[5].shape[1]) // HEAD_DIM
        parts = math.gcd(heads // math.gcd(heads, tp), sp)
        fine = Mesh(mesh.devices.reshape(sp // parts, parts, tp), ("t", "h", "tp"))
        seq = ("t", "h")
        body = jax.shard_map(
            shards,
            mesh=fine,
            in_specs=(P(seq, "tp"), P("tp"))
            + (P(seq, "tp"),) * 6
            + (P("tp", seq), P("tp", seq), P("tp"), P("tp", seq)),
            out_specs=(P(("t", "h", "tp"), None), P("tp", seq)),
            check_vma=False,
        )
        return body(*args)

    return run
```

```python
import functools
import math

import jax
import jax.numpy as jnp
from jax import lax
from jax.experimental import pallas as pl
from jax.experimental.pallas import tpu as pltpu
from jax.sharding import Mesh
from jax.sharding import PartitionSpec as P

HEAD_DIM = 128
SPAN_RADIUS = 128
BLOCK = 256
HIGHEST = lax.Precision.HIGHEST
MESH = pl.DeviceIdType.MESH


def gather(x, axis, dim):
    if lax.axis_size(axis) == 1:
        return x
    return lax.all_gather(x, axis, axis=dim, tiled=True)


def exchange(x, axis, split, concat):
    if lax.axis_size(axis) == 1:
        return x
    return lax.all_to_all(x, axis, split, concat, tiled=True)


def halo(shard, axis, width):
    peers, length = lax.axis_size(axis), shard.shape[1]
    up = [(i, i + 1) for i in range(peers - 1)]
    down = [(j, i) for i, j in up]
    before = lax.ppermute(shard[:, length - width :], axis, up)
    after = lax.ppermute(shard[:, :width], axis, down)
    return jnp.concatenate([before, shard, after], axis=1)


def rotate(values, cosine, sine):
    half = values.shape[-1] // 2
    first, second = values[..., :half], values[..., half:]
    return jnp.concatenate(
        [first * cosine - second * sine, second * cosine + first * sine], axis=-1
    ).astype(jnp.bfloat16)


def front_kernel(
    peers, parts, cores,
    packed, scaled, sums, outp, decay,
    proj, out_all, sums_all, decay_all,
    wide, seen,
    w_recv, up_send, down_send, w_send,
    x_recv, x_send, swap_send,
    s_recv, s_send, o_recv, o_send, d_recv, d_send, local,
):
    t, h, c = lax.axis_index("t"), lax.axis_index("h"), lax.axis_index("tp")
    blocks, own, _ = scaled.shape

    def other(d):
        return lax.rem(h + d, parts)

    def source(d):
        return lax.rem(h - d + parts, parts)

    barrier = pltpu.get_barrier_semaphore()
    for d in range(parts):
        for e in range(cores):
            if d or e:
                pl.semaphore_signal(
                    barrier,
                    inc=1,
                    device_id={"h": other(d), "tp": lax.rem(c + e, cores)},
                    device_id_type=MESH,
                )

    for d in range(1, peers):
        pl.semaphore_signal(
            barrier, inc=1, device_id={"t": lax.rem(t + d, peers)}, device_id_type=MESH
        )
    pl.semaphore_wait(barrier, parts * cores + peers - 2)

    def remote(src, dst, send, recv, where):
        return pltpu.make_async_remote_copy(
            src_ref=src, dst_ref=dst, send_sem=send, recv_sem=recv,
            device_id=where, device_id_type=MESH,
        )

    def upward(b, p, src=None):
        return remote(
            wide.at[b, p] if src is None else src,
            wide.at[b, p], up_send.at[b, p], w_recv.at[b, p], {"t": t + 1},
        )

    def downward(b, p, src=None):
        return remote(
            wide.at[b, p] if src is None else src,
            wide.at[b, p], down_send.at[b, p], w_recv.at[b, p], {"t": t - 1},
        )

    def weight_to(d):
        return remote(
            packed.at[other(d)], wide.at[t, h], w_send.at[d], w_recv.at[t, h], {"h": other(d)}
        )

    def place(p, e):
        return seen.at[pl.ds(e * blocks, blocks), pl.ds(p * own, own)]

    def token_to(d):
        return remote(scaled, place(h, c), x_send.at[d], x_recv.at[h, c], {"h": other(d)})

    def swap(p, src):
        return remote(
            src, place(p, c), swap_send.at[p], x_recv.at[p, c], {"tp": lax.rem(c + 1, cores)}
        )

    def sum_to(d, e):
        return remote(
            sums, sums_all.at[h, c], s_send.at[d, e], s_recv.at[h, c],
            {"h": other(d), "tp": lax.rem(c + e, cores)},
        )

    def out_to(d):
        return remote(
            outp.at[other(d)], out_all.at[h], o_send.at[d], o_recv.at[h], {"h": other(d)}
        )

    def decay_to(d):
        return remote(
            decay.at[other(d)], decay_all.at[h], d_send.at[d], d_recv.at[h], {"h": other(d)}
        )

    for d in range(1, parts):
        weight_to(d).start()

    @pl.when(t < peers - 1)
    def _():
        upward(t, h, packed.at[h]).start()

    @pl.when(t > 0)
    def _():
        downward(t, h, packed.at[h]).start()

    for d in range(1, parts):
        token_to(d).start()
    swap(h, scaled).start()
    for d in range(1, parts):
        decay_to(d).start()
        out_to(d).start()
    for d in range(parts):
        for e in range(cores):
            if d or e:
                sum_to(d, e).start()
    mine = (
        pltpu.make_async_copy(packed.at[h], wide.at[t, h], local.at[0]),
        pltpu.make_async_copy(scaled, place(h, c), local.at[1]),
        pltpu.make_async_copy(sums, sums_all.at[h, c], local.at[2]),
        pltpu.make_async_copy(outp.at[h], out_all.at[h], local.at[3]),
        pltpu.make_async_copy(decay.at[h], decay_all.at[h], local.at[4]),
    )
    for copy in mine:
        copy.start()
    proj[...] = jnp.zeros_like(proj)

    @pl.loop(1, parts)
    def _(d):
        p = source(d)
        upward(t, p).wait_recv()

        @pl.when(t < peers - 1)
        def _():
            upward(t, p).start()

        @pl.when(t > 0)
        def _():
            downward(t, p).start()

    def relay(s, d):
        p = source(d)

        @pl.when(t - s >= 0)
        def _():
            upward(t - s, p).wait_recv()

            @pl.when(t < peers - 1)
            def _():
                upward(t - s, p).start()

        @pl.when(t + s < peers)
        def _():
            downward(t + s, p).wait_recv()

            @pl.when(t > 0)
            def _():
                downward(t + s, p).start()

    @pl.loop(0, parts)
    def _(d):
        relay(1, d)

        @pl.when(d < parts - 1)
        def _():
            p = source(d + 1)
            swap(p, place(p, c)).wait_recv()
            swap(p, place(p, c)).start()

    for copy in mine:
        copy.wait()

    @pl.loop(0, parts)
    def _(p):
        e = lax.rem(c + 1, cores)
        pltpu.make_async_remote_copy(
            src_ref=place(p, e), dst_ref=place(p, e),
            send_sem=swap_send.at[p], recv_sem=x_recv.at[p, e],
            device_id={"tp": e}, device_id_type=MESH,
        ).wait_recv()

    def add(b, p):
        @pl.loop(0, parts)
        def _(r):
            at = pl.ds(pl.multiple_of(r * own, own), own)
            proj[at, :] += jnp.dot(
                seen[b * parts + p, at, :], wide[b, p], preferred_element_type=jnp.float32
            )

    @pl.loop(0, peers)
    def _(s):
        @pl.loop(0, parts)
        def _(d):
            p = source(d)

            @pl.when(s >= 2)
            def _():
                relay(s, d)

            @pl.when(t - s >= 0)
            def _():
                add(t - s, p)

            @pl.when((s > 0) & (t + s < peers))
            def _():
                add(t + s, p)

    @pl.loop(0, peers)
    def _(b):
        @pl.loop(0, parts)
        def _(p):
            @pl.when((b <= t) & (t < peers - 1))
            def _():
                upward(b, p).wait_send()

            @pl.when((b >= t) & (t > 0))
            def _():
                downward(b, p).wait_send()

    for p in range(parts):
        swap(p, place(p, c)).wait_send()
    for d in range(parts):
        if d:
            p = source(d)
            weight_to(d).wait_send()
            token_to(d).wait_send()
            out_to(d).wait_send()
            decay_to(d).wait_send()
            remote(
                outp.at[h], out_all.at[p], o_send.at[d], o_recv.at[p], {"h": p}
            ).wait_recv()
            remote(
                decay.at[h], decay_all.at[p], d_send.at[d], d_recv.at[p], {"h": p}
            ).wait_recv()
        for e in range(cores):
            if d or e:
                p, q = source(d), lax.rem(c + e, cores)
                sum_to(d, e).wait_send()
                remote(
                    sums, sums_all.at[p, q], s_send.at[d, e], s_recv.at[p, q],
                    {"h": p, "tp": q},
                ).wait_recv()


def front(packed, scaled, sums, outp, decay):
    peers, parts, cores = (lax.axis_size(a) for a in ("t", "h", "tp"))
    own, columns = packed.shape[1:]
    dma = pltpu.SemaphoreType.DMA
    vmem = pl.BlockSpec(memory_space=pltpu.VMEM)
    rows = parts * own
    return pl.pallas_call(
        functools.partial(front_kernel, peers, parts, cores),
        out_shape=(
            jax.ShapeDtypeStruct((rows, columns), jnp.float32),
            jax.ShapeDtypeStruct(outp.shape, outp.dtype),
            jax.ShapeDtypeStruct((parts, cores) + sums.shape, sums.dtype),
            jax.ShapeDtypeStruct(decay.shape, decay.dtype),
        ),
        in_specs=[vmem] * 5,
        out_specs=[vmem] * 4,
        scratch_shapes=[
            pltpu.VMEM((peers, parts, own, columns), jnp.bfloat16),
            pltpu.VMEM((cores * scaled.shape[0], rows, own), jnp.bfloat16),
            dma((peers, parts)), dma((peers, parts)), dma((peers, parts)), dma((parts,)),
            dma((parts, cores)), dma((parts,)), dma((parts,)),
            dma((parts, cores)), dma((parts, cores)),
            dma((parts,)), dma((parts,)), dma((parts,)), dma((parts,)), dma((5,)),
        ],
        compiler_params=pltpu.CompilerParams(
            collective_id=0, has_side_effects=True, vmem_limit_bytes=56 * 2**20
        ),
        cost_estimate=pl.CostEstimate(
            flops=10**11, bytes_accessed=2 * 10**7, transcendentals=0
        ),
    )(packed, scaled, sums, outp, decay)


def back_kernel(
    parts, cores, mixers, wide, logs, mixed, logs_all,
    give, take, mine, total, seen,
    give_send, take_recv, total_send, seen_recv, l_send, l_recv, local,
):
    h, c = lax.axis_index("h"), lax.axis_index("tp")
    partner = lax.rem(c + 1, cores)
    half = mixed.shape[0]
    count, _, tile = wide.shape

    def other(d):
        return lax.rem(h + d, parts)

    barrier = pltpu.get_barrier_semaphore()
    for d in range(1, parts):
        pl.semaphore_signal(barrier, inc=1, device_id={"h": other(d)}, device_id_type=MESH)
    pl.semaphore_signal(barrier, inc=1, device_id={"tp": partner}, device_id_type=MESH)
    pl.semaphore_wait(barrier, parts)

    def remote(src, dst, send, recv, where):
        return pltpu.make_async_remote_copy(
            src_ref=src, dst_ref=dst, send_sem=send, recv_sem=recv,
            device_id=where, device_id_type=MESH,
        )

    def swap(d):
        return remote(give.at[d], take.at[d], give_send.at[d], take_recv.at[d], {"tp": partner})

    def scatter(d):
        return remote(
            total.at[d], seen.at[d], total_send.at[d], seen_recv.at[d], {"h": other(d)}
        )

    def log_to(d):
        return remote(
            logs.at[other(d)], logs_all.at[h], l_send.at[d], l_recv.at[h], {"h": other(d)}
        )

    for d in range(1, parts):
        log_to(d).start()
    own_logs = pltpu.make_async_copy(logs.at[h], logs_all.at[h], local.at[0])
    own_logs.start()

    def project(d):
        at = pl.ds(pl.multiple_of(other(d) * 2 * half, 2 * half), 2 * half)

        @pl.loop(0, count)
        def _(j):
            columns = pl.ds(pl.multiple_of(j * tile, tile), tile)
            part = jnp.dot(mixers[at, :], wide[j], preferred_element_type=jnp.float32)
            low, high = part[:half], part[half:]
            give[d, :, columns] = jnp.where(c == 0, high, low).astype(give.dtype)
            mine[d, :, columns] = jnp.where(c == 0, low, high)

    def settle(d):
        swap(d).wait_recv()
        total[d] = (mine[d] + take[d].astype(jnp.float32)).astype(total.dtype)
        scatter(d).start()

    @pl.loop(1, parts + 1)
    def _(i):
        d = lax.rem(i, parts)
        project(d)
        swap(d).start()

        @pl.when(i > 1)
        def _():
            settle(i - 1)

    swap(0).wait_recv()
    mine[0] = mine[0] + take[0].astype(jnp.float32)

    @pl.loop(1, parts)
    def _(d):
        scatter(d).wait_recv()
        mine[0] += seen[d].astype(jnp.float32)

    mixed[...] = mine[0].astype(mixed.dtype)

    own_logs.wait()
    for d in range(parts):
        swap(d).wait_send()
        if d:
            scatter(d).wait_send()
            log_to(d).wait_send()
            p = lax.rem(h - d + parts, parts)
            remote(
                logs.at[h], logs_all.at[p], l_send.at[d], l_recv.at[p], {"h": p}
            ).wait_recv()


def back(mixers, wide, logs):
    parts, cores = lax.axis_size("h"), lax.axis_size("tp")
    half = mixers.shape[0] // parts // cores
    columns = wide.shape[0] * wide.shape[2]
    dma = pltpu.SemaphoreType.DMA
    vmem = pl.BlockSpec(memory_space=pltpu.VMEM)
    block = (parts, half, columns)
    return pl.pallas_call(
        functools.partial(back_kernel, parts, cores),
        out_shape=(
            jax.ShapeDtypeStruct((half, columns), jnp.bfloat16),
            jax.ShapeDtypeStruct(logs.shape, logs.dtype),
        ),
        in_specs=[vmem] * 3,
        out_specs=[vmem] * 2,
        scratch_shapes=[
            pltpu.VMEM(block, jnp.bfloat16), pltpu.VMEM(block, jnp.bfloat16),
            pltpu.VMEM(block, jnp.float32),
            pltpu.VMEM(block, jnp.bfloat16), pltpu.VMEM(block, jnp.bfloat16),
        ]
        + [dma((parts,))] * 6
        + [dma((1,))],
        compiler_params=pltpu.CompilerParams(
            collective_id=1, has_side_effects=True, vmem_limit_bytes=56 * 2**20
        ),
        cost_estimate=pl.CostEstimate(
            flops=5 * 10**10, bytes_accessed=2 * 10**7, transcendentals=0
        ),
    )(mixers, wide, logs)


def attend(query, key, value, sink, offset, total_rows):
    rows, kv, group, _ = query.shape
    ext = halo(jnp.stack([key, value]), "t", SPAN_RADIUS)
    size = min(rows, BLOCK)
    count = rows // size
    span = size + 2 * SPAN_RADIUS
    pieces = jnp.stack([ext[:, b * size : b * size + span] for b in range(count)])
    blocks = query.reshape(count, size, kv, group, HEAD_DIM)
    scores = jnp.einsum(
        "bqhgd,bkhd->bhgqk", blocks, pieces[:, 0], preferred_element_type=jnp.float32
    ) * HEAD_DIM ** (-0.5)
    base = offset + jnp.arange(count, dtype=jnp.int32) * size
    query_pos = base[:, None] + jnp.arange(size, dtype=jnp.int32)
    key_pos = base[:, None] - SPAN_RADIUS + jnp.arange(span, dtype=jnp.int32)
    spacing = key_pos[:, None, :] - query_pos[:, :, None]
    inside = (key_pos >= 0) & (key_pos < total_rows)
    valid = (jnp.abs(spacing) <= SPAN_RADIUS) & inside[:, None, :]
    masked = jnp.where(valid[:, None, None], scores, -jnp.inf)
    limit = sink[None, :, :, None]
    top = jnp.maximum(jnp.max(masked, axis=-1), limit)
    expo = jnp.exp(masked - top[..., None])
    total = jnp.sum(expo, axis=-1) + jnp.exp(limit - top)
    logs = top + jnp.log(total)
    probs = (expo / total[..., None]).astype(jnp.bfloat16)
    result = jnp.einsum(
        "bhgqk,bkhd->bqhgd", probs, pieces[:, 1], preferred_element_type=jnp.float32
    ).astype(jnp.bfloat16)
    logs = jnp.transpose(logs, (1, 2, 0, 3)).reshape(kv * group, rows)
    return result.reshape(rows, kv * group * HEAD_DIM), logs


def retain(query, key, value, decay):
    rows, heads, _ = query.shape
    peers, index = lax.axis_size("t"), lax.axis_index("t")
    cumul = jnp.cumsum(decay, axis=1)
    last = cumul[:, -1]
    query_f, key_f, value_f = (v.astype(jnp.float32) for v in (query, key, value))
    trailing = jnp.exp(last[:, None] - cumul)
    leading = jnp.exp(cumul)
    forward = jnp.einsum("hk,khd,khe->hde", trailing, key_f, value_f, precision=HIGHEST)
    backward = jnp.einsum("hk,khd,khe->hde", leading, key_f, value_f, precision=HIGHEST)
    tail = jnp.broadcast_to(last[:, None, None], (heads, 8, HEAD_DIM))
    sent = jnp.concatenate([forward, backward, tail], axis=1)
    seen = lax.all_gather(sent, "t", axis=0)
    lasts = seen[:, :, 2 * HEAD_DIM, 0]
    at = jnp.arange(peers)
    low = jnp.minimum(at, index)[:, None]
    high = jnp.maximum(at, index)[:, None]
    between = (at[None, :] > low) & (at[None, :] < high)
    spans = jnp.exp(jnp.sum(jnp.where(between[:, :, None], lasts[None], 0.0), axis=1))
    before = jnp.sum(
        jnp.where(at < index, 1.0, 0.0)[:, None, None, None]
        * spans[:, :, None, None]
        * seen[:, :, :HEAD_DIM],
        axis=0,
    )
    after = jnp.sum(
        jnp.where(at > index, 1.0, 0.0)[:, None, None, None]
        * spans[:, :, None, None]
        * seen[:, :, HEAD_DIM : 2 * HEAD_DIM],
        axis=0,
    )
    scores = jnp.einsum("qhd,khd->hqk", query, key, preferred_element_type=jnp.float32)
    weights = jnp.exp(-jnp.abs(cumul[:, :, None] - cumul[:, None, :]))
    mix = jnp.einsum("hqk,khd->qhd", scores * weights, value_f, precision=HIGHEST)
    mix = mix + leading.T[:, :, None] * jnp.einsum(
        "qhd,hde->qhe", query_f, before, precision=HIGHEST
    )
    mix = mix + trailing.T[:, :, None] * jnp.einsum(
        "qhd,hde->qhe", query_f, after, precision=HIGHEST
    )
    middle = mix - jnp.mean(mix, axis=-1, keepdims=True)
    normed = middle * lax.rsqrt(jnp.mean(middle * middle, axis=-1, keepdims=True) + 1e-06)
    return normed.astype(jnp.bfloat16).reshape(rows, heads * HEAD_DIM)


def shards(
    tokens, gain, q_att, k_att, v_att, q_ret, k_ret, v_ret, out_att, out_ret, sink, decay_log
):
    parts = lax.axis_size("h")
    own = tokens.shape[0]
    rows = own * parts
    width = tokens.shape[1] * lax.axis_size("tp")
    kv = k_att.shape[1] // HEAD_DIM // parts
    group = q_att.shape[1] // k_att.shape[1]
    att = kv * group
    ret = q_ret.shape[1] // HEAD_DIM // parts
    offset = lax.axis_index("t") * rows
    total_rows = rows * lax.axis_size("t")

    packed = jnp.concatenate(
        [
            w.reshape(w.shape[0], parts, w.shape[1] // parts)
            for w in (q_att, k_att, v_att, q_ret, k_ret, v_ret)
        ],
        axis=2,
    )
    packed = jnp.moveaxis(packed, 1, 0)
    out_pack = jnp.concatenate(
        [w.reshape(parts, w.shape[0] // parts, w.shape[1]) for w in (out_att, out_ret)], axis=1
    )
    widened = tokens.astype(jnp.float32)
    sums = jnp.sum(widened * widened, axis=1)
    scaled = (widened * gain).astype(jnp.bfloat16)
    cores = lax.axis_size("tp")
    fused = parts > 1 and cores == 2 and own % 128 == 0 and packed.shape[1] == own
    if fused:
        tiles = jnp.moveaxis(scaled.reshape(own, -1, own), 1, 0)
        proj, out_own, sums, decay = front(
            packed, tiles, sums.reshape(-1, 128), out_pack, decay_log.reshape(parts, ret, own)
        )
        decay = jnp.moveaxis(decay, 0, 1).reshape(ret, rows)
    else:
        flat = packed.reshape(parts * packed.shape[1], packed.shape[2])
        weight = gather(exchange(flat, "h", 0, 0), "t", 0)
        whole = gather(gather(scaled, "h", 0), "tp", 1)
        proj = jnp.dot(whole, weight, preferred_element_type=jnp.float32)
        out_own = exchange(out_pack, "h", 0, 0)
        sums = lax.all_gather(sums, ("h", "tp"))
        decay = exchange(decay_log, "h", 0, 1)
    squares = jnp.sum(sums.reshape(parts, cores, own), axis=1).reshape(rows)
    inverse = lax.rsqrt(squares / width + 1e-06)[:, None]

    edges = [att, kv, kv, ret, ret, ret]
    starts = [sum(edges[:i]) * HEAD_DIM for i in range(6)]
    qa, ka, va, qr, kr, vr = (
        proj[:, s : s + n * HEAD_DIM].reshape(rows, n, HEAD_DIM) for s, n in zip(starts, edges)
    )
    scale = inverse[:, :, None]
    positions = (offset + jnp.arange(rows, dtype=jnp.int32)).astype(jnp.float32)
    freqs = 10000.0 ** (-jnp.arange(0, HEAD_DIM, 2).astype(jnp.float32) / HEAD_DIM)
    angles = positions[:, None] * freqs[None, :]
    cosine, sine = jnp.cos(angles)[:, None, :], jnp.sin(angles)[:, None, :]
    att_query = rotate(qa * scale, cosine, sine)
    att_key = rotate(ka * scale, cosine, sine)
    att_value = (va * scale).astype(jnp.bfloat16)
    ret_query = (qr * scale).astype(jnp.bfloat16)
    ret_key = (kr * (scale * HEAD_DIM ** (-0.5))).astype(jnp.bfloat16)
    ret_value = (vr * scale).astype(jnp.bfloat16)

    logits = lax.dynamic_slice_in_dim(sink, lax.axis_index("h") * att, att).reshape(kv, group)
    att_out, logs = attend(
        att_query.reshape(rows, kv, group, HEAD_DIM), att_key, att_value, logits, offset, total_rows
    )
    ret_out = retain(ret_query, ret_key, ret_value, decay)

    out_wide = gather(out_own, "t", 0)
    mixers = jnp.concatenate([att_out, ret_out], axis=1)
    if fused:
        sent = jnp.moveaxis(logs.reshape(att, parts, own), 1, 0)
        mixed, seen = back(mixers, out_wide, sent)
        return mixed, seen.reshape(parts * att, own)
    depth = out_wide.shape[1]
    out_wide = jnp.moveaxis(out_wide, 0, 1).reshape(depth, -1)
    mixed = jnp.dot(mixers, out_wide, preferred_element_type=jnp.float32).astype(jnp.bfloat16)
    mixed = lax.psum_scatter(mixed, ("h", "tp"), scatter_dimension=0, tiled=True)
    return mixed, exchange(logs, "h", 1, 0)


def solution(mesh):
    sp, tp = mesh.shape["sp"], mesh.shape["tp"]

    def run(*args):
        heads = math.gcd(args[3].shape[1], args[5].shape[1]) // HEAD_DIM
        parts = math.gcd(heads // math.gcd(heads, tp), sp)
        fine = Mesh(mesh.devices.reshape(sp // parts, parts, tp), ("t", "h", "tp"))
        seq = ("t", "h")
        body = jax.shard_map(
            shards,
            mesh=fine,
            in_specs=(P(seq, "tp"), P("tp"))
            + (P(seq, "tp"),) * 6
            + (P("tp", seq), P("tp", seq), P("tp"), P("tp", seq)),
            out_specs=(P(("t", "h", "tp"), None), P("tp", seq)),
            check_vma=False,
        )
        return body(*args)

    return run
```
